256 devices in a mesh: sp: 64 (over z, x, core), tp: 4 (over y).
Axes of the slice: x: 4, y: 4, z: 8, core: 2. Of those that a mesh axis runs over, the one named last changes fastest.
Arguments:
- queries: bfloat16 [32768, 2048], P('sp', 'tp'), may hold values from -90 to 90, as said below
- key_rows: bfloat16 [32768, 512], P('sp', 'tp'), may hold values from -6 to 6
- value_rows: bfloat16 [32768, 512], P('sp', 'tp'), may hold values from -6 to 6
- sink_logits: float32 [16], P('tp'), may hold values from 2 to 7
- residual: bfloat16 [32768, 2048], P('sp'), may hold values from -6 to 6
- norm_gain: float32 [2048], replicated, may hold values from 0.1 to 1.9
- out_weight: bfloat16 [2048, 2048], P('tp'), may hold values from -1.5 to 1.5
- gate_weight: bfloat16 [2048, 5632], P('sp', 'tp'), may hold values from -0.125 to 0.125
- up_weight: bfloat16 [2048, 5632], P('sp', 'tp'), may hold values from -0.125 to 0.125
- down_weight: bfloat16 [5632, 2048], P('tp', 'sp'), may hold values from -0.078125 to 0.078125
Outputs:
- mixed: bfloat16 [32768, 2048], P(('sp', 'tp'))
The draws below stay inside these ranges and needn't reach their ends.
Inputs may be any that keep to these rules, and one draw needn't show every extreme that they name: queries are mostly of order one; some rows may be much larger.
All inputs are finite; a program needn't handle non-finite values.
Results may differ from the reference program's by a relative error of at most 0.012.
Values may be sent and summed in bfloat16 or wider, within the bound.
No kernel may reach another device: no remote copies, remote signals or barrier semaphores. Data moves between devices by JAX's collectives and lax.ppermute only.
A program may use at most 128 MiB of HBM per device.

```python
import jax
import jax.numpy as jnp
from jax import lax

D = 2048
HQ = 16
HK = 4
DH = 128
FF = 5632
WIN = 128
TOKENS = 32768
N_TP = 4


def shared_draws(key):
    base = jax.random.fold_in(key, 11)
    key_query, key_keys = jax.random.split(base, 2)
    keys_wide = jnp.clip(jax.random.normal(key_keys, (TOKENS, HK * DH), jnp.float32), -5.0, 5.0)
    query_wide = jnp.clip(jax.random.normal(key_query, (TOKENS, HQ * DH), jnp.float32), -5.0, 5.0)
    return (query_wide, keys_wide)


def draw_queries(key, part):
    return shared_draws(key)[0].astype(jnp.bfloat16)


def draw_key_rows(key, part):
    return shared_draws(key)[1].astype(jnp.bfloat16)


def steps_of(stream_key, shape, cuts, smallest, largest):
    def one(position, shards_of):
        steps = jax.random.uniform(jax.random.fold_in(jax.random.fold_in(stream_key, 6), position), (shards_of,), jnp.float32, smallest / len(cuts), largest / len(cuts))
        return jnp.repeat(jnp.exp(steps), shape[position] // shards_of).reshape((-1,) + (1,) * (len(shape) - position - 1))

    factor_of = one(*cuts[0])
    for cut in cuts[1:]:
        factor_of = factor_of * one(*cut)
    return factor_of


def gaussian(stream_key, dims, spread, most, pieces=(), kind=jnp.bfloat16):
    level = steps_of(stream_key, dims, pieces, -0.22, 0.18) if pieces else 1.0
    values = jax.random.normal(stream_key, dims, jnp.float32) * spread * level
    return jnp.minimum(jnp.maximum(values, -most), most).astype(kind)


def setup_inputs(seed: int = 0) -> dict:
    key_of = jax.random.split(jax.random.key(seed), 11)
    return {
        "queries": draw_queries(jax.random.fold_in(key_of[10], 71), 0),
        "key_rows": draw_key_rows(jax.random.fold_in(key_of[10], 71), 0),
        "value_rows": gaussian(key_of[2], (TOKENS, HK * DH), 1.0, 6.0, ((0, 64), (1, 4))),
        "sink_logits": jnp.clip(2.0 + 5.0 * jax.random.uniform(key_of[3], (HQ,), jnp.float32) ** steps_of(key_of[3], (HQ,), ((0, 4),), -0.2, 0.2), 2.0, 7.0),
        "residual": gaussian(key_of[4], (TOKENS, D), 1.0, 6.0, ((0, 64),)),
        "norm_gain": jnp.clip(1.0 + 0.18 * jax.random.normal(key_of[5], (D,), jnp.float32), 0.1, 1.9),
        "out_weight": gaussian(key_of[6], (HQ * DH, D), 0.25, 1.5, ((0, 4),)),
        "gate_weight": gaussian(key_of[7], (D, FF), D ** -0.5, 0.125, ((0, 64), (1, 4))),
        "up_weight": gaussian(key_of[8], (D, FF), D ** -0.5, 0.125, ((0, 64), (1, 4))),
        "down_weight": gaussian(key_of[9], (FF, D), FF ** -0.5, 0.078125, ((0, 4), (1, 64))),
    }


EPSILON = 1e-06
MASKED = -1e+30

def attend_block(query_blk, key_blk, value_blk, sink_logits, query_pos, key_pos, seq_len):
    kv_heads = key_blk.shape[1] // DH
    group_size = query_blk.shape[1] // key_blk.shape[1]
    query_four = query_blk.reshape(query_blk.shape[0], kv_heads, group_size, DH).astype(jnp.float32)
    key_three = key_blk.reshape(key_blk.shape[0], kv_heads, DH).astype(jnp.float32)
    value_three = value_blk.reshape(value_blk.shape[0], kv_heads, DH).astype(jnp.float32)
    scores = jnp.einsum('qhgd,khd->hgqk', query_four, key_three) * DH ** (-0.5)
    allowed = (jnp.abs(key_pos[None, :] - query_pos[:, None]) <= WIN) & (key_pos[None, :] >= 0) & (key_pos[None, :] < seq_len)
    scores = jnp.where(allowed[None, None], scores, MASKED)
    sink_col = sink_logits.astype(jnp.float32).reshape(kv_heads, group_size)[:, :, None]
    highest = jnp.maximum(lax.optimization_barrier(jnp.max(scores, axis=-1)), sink_col)
    weights_exp = jnp.exp(scores - highest[..., None])
    denominator = lax.optimization_barrier(jnp.sum(weights_exp, axis=-1)) + jnp.exp(sink_col - highest)
    probabilities = (weights_exp / denominator[..., None]).astype(jnp.bfloat16)
    heads_out = jnp.einsum('hgqk,khd->qhgd', probabilities.astype(jnp.float32), value_three)
    return heads_out.astype(jnp.bfloat16).reshape(query_blk.shape[0], kv_heads * group_size * DH)

def rms_scale(rows_wide, norm_gain):
    mean_square = lax.optimization_barrier(jnp.mean(rows_wide * rows_wide, axis=-1, keepdims=True))
    return (rows_wide * lax.rsqrt(mean_square + EPSILON) * norm_gain).astype(jnp.bfloat16)

def grouped_sum(left, right, group_cols):
    result = jnp.zeros((left.shape[0], right.shape[1]), jnp.float32)
    for group_index in range(N_TP):
        lower = group_index * group_cols
        partial_term = jnp.dot(left[:, lower:lower + group_cols], right[lower:lower + group_cols], preferred_element_type=jnp.float32)
        rounded = lax.optimization_barrier(partial_term.astype(jnp.bfloat16))
        result = result + rounded.astype(jnp.float32)
    return result

def reference(queries, key_rows, value_rows, sink_logits, residual, norm_gain, out_weight, gate_weight, up_weight, down_weight):
    block_len = 2 * WIN
    key_pad = jnp.pad(key_rows, ((WIN, WIN), (0, 0)))
    value_pad = jnp.pad(value_rows, ((WIN, WIN), (0, 0)))

    def one_block(block_index):
        block_first = (block_index * block_len).astype(jnp.int32)
        query_blk = lax.dynamic_slice_in_dim(queries, block_first, block_len, 0)
        key_blk = lax.dynamic_slice_in_dim(key_pad, block_first, block_len + 2 * WIN, 0)
        value_blk = lax.dynamic_slice_in_dim(value_pad, block_first, block_len + 2 * WIN, 0)
        query_pos = block_first + jnp.arange(block_len, dtype=jnp.int32)
        key_pos = block_first - WIN + jnp.arange(block_len + 2 * WIN, dtype=jnp.int32)
        return attend_block(query_blk, key_blk, value_blk, sink_logits, query_pos, key_pos, TOKENS)
    blocks = lax.map(one_block, jnp.arange(TOKENS // block_len, dtype=jnp.int32))
    attended = blocks.reshape(TOKENS, HQ * DH)
    attn_total = grouped_sum(attended, out_weight, HQ * DH // N_TP)
    middle = residual.astype(jnp.float32) + attn_total
    normed = rms_scale(middle, norm_gain)
    gate_acc = jnp.dot(normed, gate_weight, preferred_element_type=jnp.float32)
    up_acc = jnp.dot(normed, up_weight, preferred_element_type=jnp.float32)
    hidden = (jax.nn.silu(gate_acc) * up_acc).astype(jnp.bfloat16)
    ffn_total = grouped_sum(hidden, down_weight, FF // N_TP)
    return (middle + ffn_total).astype(jnp.bfloat16)
```

```python
import jax
import jax.numpy as jnp
from jax import lax
from jax.sharding import PartitionSpec as P

DH = 128
WIN = 128


EPSILON = 1e-06
MASKED = -1e30


def with_halo(cells, sides, width):
    for axis, dim in sides:
        count = lax.axis_size(axis)
        ends = count - 1
        head = lax.slice_in_dim(cells, 0, width, axis=dim)
        tail = lax.slice_in_dim(cells, cells.shape[dim] - width, cells.shape[dim], axis=dim)
        cells = jnp.concatenate(
            [
                lax.ppermute(tail, axis, [(i, (i + 1) % count) for i in range(ends)]),
                cells,
                lax.ppermute(head, axis, [((i + 1) % count, i) for i in range(ends)]),
            ],
            axis=dim,
        )
    return cells


def split_up(value, dim, size):
    before, after = (value.shape[:dim], value.shape[dim + 1 :])
    return jnp.moveaxis(value.reshape(*before, size, -1, *after), dim, 0)


def sent_and_summed(value, axis, dim):
    size = lax.axis_size(axis)
    blocks = lax.all_to_all(split_up(value, dim, size), axis, 0, 0, tiled=True)
    return jnp.sum(blocks.astype(jnp.float32), axis=0)


def sent_to_all(value, axis):
    size = lax.axis_size(axis)
    return lax.all_to_all(
        jnp.broadcast_to(value[None], (size, *value.shape)), axis, 0, 0, tiled=True
    )


def laid_out(blocks, dim):
    blocks = jnp.moveaxis(blocks, 0, dim)
    lengths = blocks.shape
    return blocks.reshape(*lengths[:dim], lengths[dim] * lengths[dim + 1], *lengths[dim + 2 :])


def gather_directly(value, axis, dim):
    blocks = sent_to_all(value, axis)
    return laid_out(blocks, dim)


def side_by_side(arrays, axis, dim, along):
    ends, at = ([], 0)
    for a in arrays[:-1]:
        at += a.shape[along]
        ends.append(at)
    both = jnp.concatenate(arrays, axis=along)
    return tuple(jnp.split(lax.all_gather(both, axis, axis=dim, tiled=True), ends, axis=along))


def attend_block(query_blk, key_blk, value_blk, sink_logits, query_pos, key_pos, seq_len):
    kv_heads = key_blk.shape[1] // DH
    group_size = query_blk.shape[1] // key_blk.shape[1]
    query_four = query_blk.reshape(query_blk.shape[0], kv_heads, group_size, DH)
    key_three = key_blk.reshape(key_blk.shape[0], kv_heads, DH)
    value_three = value_blk.reshape(value_blk.shape[0], kv_heads, DH)
    scores = jnp.einsum(
        "qhgd,khd->hgqk", query_four, key_three, preferred_element_type=jnp.float32
    ) * DH ** (-0.5)
    allowed = (
        (jnp.abs(key_pos[None, :] - query_pos[:, None]) <= WIN)
        & (key_pos[None, :] >= 0)
        & (key_pos[None, :] < seq_len)
    )
    scores = jnp.where(allowed[None, None], scores, MASKED)
    sink_col = sink_logits.reshape(kv_heads, group_size)[:, :, None]
    highest = jnp.maximum(jnp.max(scores, axis=-1), sink_col)
    weights_exp = jnp.exp(scores - highest[..., None])
    denominator = jnp.sum(weights_exp, axis=-1) + jnp.exp(sink_col - highest)
    probabilities = (weights_exp / denominator[..., None]).astype(jnp.bfloat16)
    heads_out = jnp.einsum(
        "hgqk,khd->qhgd", probabilities, value_three, preferred_element_type=jnp.float32
    )
    return heads_out.astype(jnp.bfloat16).reshape(query_blk.shape[0], kv_heads * group_size * DH)


def rms_scale(rows_wide, norm_gain):
    mean_square = jnp.mean(rows_wide * rows_wide, axis=-1, keepdims=True)
    return (rows_wide * lax.rsqrt(mean_square + EPSILON) * norm_gain).astype(jnp.bfloat16)


def hop(value, step):
    size = lax.axis_size("tp")
    return lax.ppermute(value, "tp", [(i, (i + step) % size) for i in range(size)])


def ring_sum(parts):
    half = parts.shape[1] // 2
    me = lax.axis_index("tp")
    own = lax.dynamic_index_in_dim(parts, me, 0, keepdims=False)
    nxt = lax.dynamic_index_in_dim(parts, (me + 1) % 4, 0, keepdims=False)
    prv = lax.dynamic_index_in_dim(parts, (me + 3) % 4, 0, keepdims=False)
    far = lax.dynamic_index_in_dim(parts, (me + 2) % 4, 0, keepdims=False)
    up = hop(far[:half], 1)
    down = hop(far[half:], -1)
    up_sum = (nxt[:half].astype(jnp.float32) + up.astype(jnp.float32)).astype(jnp.bfloat16)
    down_sum = (prv[half:].astype(jnp.float32) + down.astype(jnp.float32)).astype(jnp.bfloat16)
    from_prev = hop(jnp.concatenate([up_sum, nxt[half:]]), 1)
    from_next = hop(jnp.concatenate([prv[:half], down_sum]), -1)
    return (
        own.astype(jnp.float32) + from_prev.astype(jnp.float32) + from_next.astype(jnp.float32)
    )


def ring_gather(own):
    half = own.shape[0] // 2
    left = hop(own, 1)
    right = hop(own, -1)
    far_a = hop(left[:half], 1)
    far_b = hop(right[half:], -1)
    far = jnp.concatenate([far_a, far_b])
    me = lax.axis_index("tp")
    rel = jnp.stack([own, right, far, left])
    return jnp.concatenate([lax.dynamic_index_in_dim(rel, (k - me) % 4, 0, keepdims=False) for k in range(4)])


def shards(
    queries,
    key_rows,
    value_rows,
    sink_logits,
    residual,
    norm_gain,
    out_weight,
    gate_weight,
    up_weight,
    down_weight,
):
    tok_local = queries.shape[0]
    block_len = 2 * WIN
    share_rows = tok_local // lax.axis_size("tp")
    seq_len = tok_local * lax.axis_size("sp")
    device_offset = lax.axis_index("sp") * tok_local
    kv_pair = jnp.stack([key_rows, value_rows])
    kv_ext = with_halo(kv_pair, (("sp", 1),), WIN)

    def one_block(block_index):
        block_first = block_index * block_len
        query_blk = lax.dynamic_slice_in_dim(queries, block_first, block_len, 0)
        key_blk = lax.dynamic_slice_in_dim(kv_ext[0], block_first, block_len + 2 * WIN, 0)
        value_blk = lax.dynamic_slice_in_dim(kv_ext[1], block_first, block_len + 2 * WIN, 0)
        query_pos = device_offset + block_first + jnp.arange(block_len, dtype=jnp.int32)
        key_pos = (
            device_offset + block_first - WIN + jnp.arange(block_len + 2 * WIN, dtype=jnp.int32)
        )
        return attend_block(query_blk, key_blk, value_blk, sink_logits, query_pos, key_pos, seq_len)

    blocks = lax.map(one_block, jnp.arange(tok_local // block_len, dtype=jnp.int32))
    attended = blocks.reshape(tok_local, queries.shape[1])
    own_first = lax.axis_index("tp") * share_rows
    picked = attended
    attn_share = ring_sum(
        jnp.dot(picked, out_weight, preferred_element_type=jnp.float32)
        .astype(jnp.bfloat16)
        .reshape(4, share_rows, -1)
    )
    middle_own = (
        lax.dynamic_slice_in_dim(residual, own_first, share_rows, 0).astype(jnp.float32)
        + attn_share
    )
    normed_all = ring_gather(rms_scale(middle_own, norm_gain))
    pieces = side_by_side((gate_weight, up_weight, down_weight.T), "sp", 0, 1)
    gate_sectioned = pieces[0]
    up_sectioned = pieces[1]
    gate_acc = jnp.dot(normed_all, gate_sectioned, preferred_element_type=jnp.float32)
    up_acc = jnp.dot(normed_all, up_sectioned, preferred_element_type=jnp.float32)
    down_whole = pieces[2]
    hidden = (jax.nn.silu(gate_acc) * up_acc).astype(jnp.bfloat16)
    picked = hidden
    ffn_share = ring_sum(
        lax.dot_general(
            picked, down_whole, (((1,), (1,)), ((), ())), preferred_element_type=jnp.float32
        )
        .astype(jnp.bfloat16)
        .reshape(4, share_rows, -1)
    )
    return (middle_own + ffn_share).astype(jnp.bfloat16)


def solution(mesh):
    placed = (
        P("sp", "tp"),
        P("sp", "tp"),
        P("sp", "tp"),
        P("tp"),
        P("sp", None),
        P(),
        P("tp", None),
        P("sp", "tp"),
        P("sp", "tp"),
        P("tp", "sp"),
    )
    return jax.shard_map(
        shards, mesh=mesh, in_specs=placed, out_specs=P(("sp", "tp"), None), check_vma=False
    )
```

```python
import jax
import jax.numpy as jnp
from jax import lax
from jax.experimental import pallas as pl
from jax.experimental.pallas import tpu as pltpu
from jax.sharding import PartitionSpec as P

DH = 128
WIN = 128


EPSILON = 1e-06
MASKED = -1e30


def with_halo(cells, sides, width):
    for axis, dim in sides:
        count = lax.axis_size(axis)
        ends = count - 1
        head = lax.slice_in_dim(cells, 0, width, axis=dim)
        tail = lax.slice_in_dim(cells, cells.shape[dim] - width, cells.shape[dim], axis=dim)
        cells = jnp.concatenate(
            [
                lax.ppermute(tail, axis, [(i, (i + 1) % count) for i in range(ends)]),
                cells,
                lax.ppermute(head, axis, [((i + 1) % count, i) for i in range(ends)]),
            ],
            axis=dim,
        )
    return cells


def attend_block(query_blk, key_blk, value_blk, sink_logits, query_pos, key_pos, seq_len):
    kv_heads = key_blk.shape[1] // DH
    group_size = query_blk.shape[1] // key_blk.shape[1]
    query_four = query_blk.reshape(query_blk.shape[0], kv_heads, group_size, DH)
    key_three = key_blk.reshape(key_blk.shape[0], kv_heads, DH)
    value_three = value_blk.reshape(value_blk.shape[0], kv_heads, DH)
    scores = jnp.einsum(
        "qhgd,khd->hgqk", query_four, key_three, preferred_element_type=jnp.float32
    ) * DH ** (-0.5)
    allowed = (
        (jnp.abs(key_pos[None, :] - query_pos[:, None]) <= WIN)
        & (key_pos[None, :] >= 0)
        & (key_pos[None, :] < seq_len)
    )
    scores = jnp.where(allowed[None, None], scores, MASKED)
    sink_col = sink_logits.reshape(kv_heads, group_size)[:, :, None]
    highest = jnp.maximum(jnp.max(scores, axis=-1), sink_col)
    weights_exp = jnp.exp(scores - highest[..., None])
    denominator = jnp.sum(weights_exp, axis=-1) + jnp.exp(sink_col - highest)
    probabilities = (weights_exp / denominator[..., None]).astype(jnp.bfloat16)
    heads_out = jnp.einsum(
        "hgqk,khd->qhgd", probabilities, value_three, preferred_element_type=jnp.float32
    )
    return heads_out.astype(jnp.bfloat16).reshape(query_blk.shape[0], kv_heads * group_size * DH)


def rms_scale(rows_wide, norm_gain):
    mean_square = jnp.mean(rows_wide * rows_wide, axis=-1, keepdims=True)
    return (rows_wide * lax.rsqrt(mean_square + EPSILON) * norm_gain).astype(jnp.bfloat16)


def hop(value, step):
    size = lax.axis_size("tp")
    return lax.ppermute(value, "tp", [(i, (i + step) % size) for i in range(size)])


def ring_sum(parts):
    half = parts.shape[1] // 2
    me = lax.axis_index("tp")
    own = lax.dynamic_index_in_dim(parts, me, 0, keepdims=False)
    nxt = lax.dynamic_index_in_dim(parts, (me + 1) % 4, 0, keepdims=False)
    prv = lax.dynamic_index_in_dim(parts, (me + 3) % 4, 0, keepdims=False)
    far = lax.dynamic_index_in_dim(parts, (me + 2) % 4, 0, keepdims=False)
    up = hop(far[:half], 1)
    down = hop(far[half:], -1)
    up_sum = (nxt[:half].astype(jnp.float32) + up.astype(jnp.float32)).astype(jnp.bfloat16)
    down_sum = (prv[half:].astype(jnp.float32) + down.astype(jnp.float32)).astype(jnp.bfloat16)
    from_prev = hop(jnp.concatenate([up_sum, nxt[half:]]), 1)
    from_next = hop(jnp.concatenate([prv[:half], down_sum]), -1)
    return (
        own.astype(jnp.float32) + from_prev.astype(jnp.float32) + from_next.astype(jnp.float32)
    )


FF_LOCAL = 1408
STEPS = ((0, 256), (256, 256), (512, 256), (768, 256), (1024, 256), (1280, 128))


def ffn_kernel(own, nxt, far_lo, far_hi, prv, w, *refs):
    outs, mine, (hidden, wg, wd, sems) = refs[:6], refs[6], refs[7:]

    def fetch(part, first, width, to, sem):
        src = w.at[:, pl.ds(part * FF_LOCAL + first, width)]
        return pltpu.make_async_copy(src, to, sem)

    copies = []
    for n, (first, width) in enumerate(STEPS):
        for part in range(2):
            to = wg.at[:, pl.ds(2 * first + part * width, width)]
            copies.append(fetch(part, first, width, to, sems.at[2 * n + part]))
    downs = fetch(2, 0, FF_LOCAL, wd, sems.at[12])
    for c in copies + [downs]:
        c.start()
    x = jnp.concatenate([far_lo[...], far_hi[...], nxt[...], prv[...], own[...]], axis=0)
    for n, (first, width) in enumerate(STEPS):
        copies[2 * n].wait()
        copies[2 * n + 1].wait()
        acc = jnp.dot(
            x, wg[:, 2 * first : 2 * (first + width)], preferred_element_type=jnp.float32
        )
        gate = acc[:, :width]
        hid = gate / (1.0 + jnp.exp(-gate)) * acc[:, width:]
        hidden[:, first : first + width] = hid.astype(jnp.bfloat16)
    downs.wait()
    res = lax.dot_general(
        hidden[...], wd[...], (((1,), (1,)), ((), ())), preferred_element_type=jnp.float32
    )
    for i, out in enumerate(outs):
        out[...] = res[64 * i : 64 * i + 64].astype(jnp.bfloat16)
    mine[...] = res[384:]


def bf16(*shape):
    return jax.ShapeDtypeStruct(shape, jnp.bfloat16)


def feed_forward(own, nxt, far_lo, far_hi, prv, weights):
    vmem = pl.BlockSpec(memory_space=pltpu.VMEM)
    hbm = pl.BlockSpec(memory_space=pltpu.HBM)
    out_lo, out_hi, nxt_lo, nxt_hi, prv_lo, prv_hi, mine = pl.pallas_call(
        ffn_kernel,
        out_shape=(bf16(64, 2048),) * 6 + (jax.ShapeDtypeStruct((128, 2048), jnp.float32),),
        in_specs=[vmem] * 5 + [hbm],
        out_specs=(vmem,) * 7,
        scratch_shapes=[
            pltpu.VMEM((512, FF_LOCAL), jnp.bfloat16),
            pltpu.VMEM((2048, 2 * FF_LOCAL), jnp.bfloat16),
            pltpu.VMEM((2048, FF_LOCAL), jnp.bfloat16),
            pltpu.SemaphoreType.DMA((13,)),
        ],
        compiler_params=pltpu.CompilerParams(vmem_limit_bytes=36 * 1024 * 1024),
        name="ffn",
    )(own, nxt, far_lo, far_hi, prv, weights)
    up, down = hop(out_lo, 1), hop(out_hi, -1)
    prev_hi, next_lo = hop(nxt_hi, 1), hop(prv_lo, -1)
    up_sum = (nxt_lo.astype(jnp.float32) + up.astype(jnp.float32)).astype(jnp.bfloat16)
    down_sum = (prv_hi.astype(jnp.float32) + down.astype(jnp.float32)).astype(jnp.bfloat16)
    prev_lo, next_hi = hop(up_sum, 1), hop(down_sum, -1)
    return mine, prev_lo, prev_hi, next_lo, next_hi


def shards(
    queries,
    key_rows,
    value_rows,
    sink_logits,
    residual,
    norm_gain,
    out_weight,
    gate_weight,
    up_weight,
    down_weight,
):
    tok_local = queries.shape[0]
    block_len = 2 * WIN
    share_rows = tok_local // lax.axis_size("tp")
    seq_len = tok_local * lax.axis_size("sp")
    device_offset = lax.axis_index("sp") * tok_local
    kv_pair = jnp.stack([key_rows, value_rows])
    kv_ext = with_halo(kv_pair, (("sp", 1),), WIN)

    def one_block(block_index):
        block_first = block_index * block_len
        query_blk = lax.dynamic_slice_in_dim(queries, block_first, block_len, 0)
        key_blk = lax.dynamic_slice_in_dim(kv_ext[0], block_first, block_len + 2 * WIN, 0)
        value_blk = lax.dynamic_slice_in_dim(kv_ext[1], block_first, block_len + 2 * WIN, 0)
        query_pos = device_offset + block_first + jnp.arange(block_len, dtype=jnp.int32)
        key_pos = (
            device_offset + block_first - WIN + jnp.arange(block_len + 2 * WIN, dtype=jnp.int32)
        )
        return attend_block(query_blk, key_blk, value_blk, sink_logits, query_pos, key_pos, seq_len)

    blocks = lax.map(one_block, jnp.arange(tok_local // block_len, dtype=jnp.int32))
    attended = blocks.reshape(tok_local, queries.shape[1])
    own_first = lax.axis_index("tp") * share_rows
    picked = attended
    attn_share = ring_sum(
        jnp.dot(picked, out_weight, preferred_element_type=jnp.float32)
        .astype(jnp.bfloat16)
        .reshape(4, share_rows, -1)
    )
    middle_own = (
        lax.dynamic_slice_in_dim(residual, own_first, share_rows, 0).astype(jnp.float32)
        + attn_share
    )
    normed = rms_scale(middle_own, norm_gain)
    prv, nxt = hop(normed, 1), hop(normed, -1)
    far_lo, far_hi = hop(prv[:64], 1), hop(nxt[64:], -1)
    weights = lax.all_gather(
        jnp.concatenate([gate_weight, up_weight, down_weight.T], axis=1), "sp", axis=0, tiled=True
    )
    mine, prev_lo, prev_hi, next_lo, next_hi = feed_forward(
        normed, nxt, far_lo, far_hi, prv, weights
    )
    ffn_share = mine + jnp.concatenate(
        [
            prev_lo.astype(jnp.float32) + next_lo.astype(jnp.float32),
            prev_hi.astype(jnp.float32) + next_hi.astype(jnp.float32),
        ]
    )
    return (middle_own + ffn_share).astype(jnp.bfloat16)


def solution(mesh):
    placed = (
        P("sp", "tp"),
        P("sp", "tp"),
        P("sp", "tp"),
        P("tp"),
        P("sp", None),
        P(),
        P("tp", None),
        P("sp", "tp"),
        P("sp", "tp"),
        P("tp", "sp"),
    )
    return jax.shard_map(
        shards, mesh=mesh, in_specs=placed, out_specs=P(("sp", "tp"), None), check_vma=False
    )
```

```python
import jax
import jax.numpy as jnp
from jax import lax
from jax.experimental import pallas as pl
from jax.experimental.pallas import tpu as pltpu
from jax.sharding import PartitionSpec as P

DH = 128
WIN = 128


EPSILON = 1e-06
MASKED = -1e30


def with_halo(cells, sides, width):
    for axis, dim in sides:
        count = lax.axis_size(axis)
        ends = count - 1
        head = lax.slice_in_dim(cells, 0, width, axis=dim)
        tail = lax.slice_in_dim(cells, cells.shape[dim] - width, cells.shape[dim], axis=dim)
        cells = jnp.concatenate(
            [
                lax.ppermute(tail, axis, [(i, (i + 1) % count) for i in range(ends)]),
                cells,
                lax.ppermute(head, axis, [((i + 1) % count, i) for i in range(ends)]),
            ],
            axis=dim,
        )
    return cells


def attend_block(query_blk, key_blk, value_blk, sink_logits, query_pos, key_pos, seq_len):
    kv_heads = key_blk.shape[1] // DH
    group_size = query_blk.shape[1] // key_blk.shape[1]
    query_four = query_blk.reshape(query_blk.shape[0], kv_heads, group_size, DH)
    key_three = key_blk.reshape(key_blk.shape[0], kv_heads, DH)
    value_three = value_blk.reshape(value_blk.shape[0], kv_heads, DH)
    scores = jnp.einsum(
        "qhgd,khd->hgqk", query_four, key_three, preferred_element_type=jnp.float32
    ) * DH ** (-0.5)
    allowed = (
        (jnp.abs(key_pos[None, :] - query_pos[:, None]) <= WIN)
        & (key_pos[None, :] >= 0)
        & (key_pos[None, :] < seq_len)
    )
    scores = jnp.where(allowed[None, None], scores, MASKED)
    sink_col = sink_logits.reshape(kv_heads, group_size)[:, :, None]
    highest = jnp.maximum(jnp.max(scores, axis=-1), sink_col)
    weights_exp = jnp.exp(scores - highest[..., None])
    denominator = jnp.sum(weights_exp, axis=-1) + jnp.exp(sink_col - highest)
    probabilities = (weights_exp / denominator[..., None]).astype(jnp.bfloat16)
    heads_out = jnp.einsum(
        "hgqk,khd->qhgd", probabilities, value_three, preferred_element_type=jnp.float32
    )
    return heads_out.astype(jnp.bfloat16).reshape(query_blk.shape[0], kv_heads * group_size * DH)


def rms_scale(rows_wide, norm_gain):
    mean_square = jnp.mean(rows_wide * rows_wide, axis=-1, keepdims=True)
    return (rows_wide * lax.rsqrt(mean_square + EPSILON) * norm_gain).astype(jnp.bfloat16)


def hop(value, step):
    size = lax.axis_size("tp")
    return lax.ppermute(value, "tp", [(i, (i + step) % size) for i in range(size)])


def ring_sum(parts):
    half = parts.shape[1] // 2
    me = lax.axis_index("tp")
    own = lax.dynamic_index_in_dim(parts, me, 0, keepdims=False)
    nxt = lax.dynamic_index_in_dim(parts, (me + 1) % 4, 0, keepdims=False)
    prv = lax.dynamic_index_in_dim(parts, (me + 3) % 4, 0, keepdims=False)
    far = lax.dynamic_index_in_dim(parts, (me + 2) % 4, 0, keepdims=False)
    up = hop(far[:half], 1)
    down = hop(far[half:], -1)
    up_sum = (nxt[:half].astype(jnp.float32) + up.astype(jnp.float32)).astype(jnp.bfloat16)
    down_sum = (prv[half:].astype(jnp.float32) + down.astype(jnp.float32)).astype(jnp.bfloat16)
    from_prev = hop(jnp.concatenate([up_sum, nxt[half:]]), 1)
    from_next = hop(jnp.concatenate([prv[:half], down_sum]), -1)
    return (
        own.astype(jnp.float32) + from_prev.astype(jnp.float32) + from_next.astype(jnp.float32)
    )


FF_LOCAL = 1408
LIMIT = 30
STEPS = ((0, 256), (256, 256), (512, 256), (768, 256), (1024, 256), (1280, 128))


def ffn_rows(x, wg, wd, hidden, ready=None):
    x = x[...]
    for n, (first, width) in enumerate(STEPS):
        if ready is not None:
            ready[2 * n].wait()
            ready[2 * n + 1].wait()
        acc = jnp.dot(
            x, wg[:, 2 * first : 2 * (first + width)], preferred_element_type=jnp.float32
        )
        gate = acc[:, :width]
        hid = gate / (1.0 + jnp.exp(-gate)) * acc[:, width:]
        hidden[:, first : first + width] = hid.astype(jnp.bfloat16)
    if ready is not None:
        ready[12].wait()
    return lax.dot_general(
        hidden[...], wd[...], (((1,), (1,)), ((), ())), preferred_element_type=jnp.float32
    )


def first_kernel(x, w, *refs):
    outs, (wg, wd, hidden, sems) = refs[:4], refs[4:]

    def fetch(part, first, width, to, sem):
        src = w.at[:, pl.ds(part * FF_LOCAL + first, width)]
        return pltpu.make_async_copy(src, to, sem)

    copies = []
    for n, (first, width) in enumerate(STEPS):
        for part in range(2):
            to = wg.at[:, pl.ds(2 * first + part * width, width)]
            copies.append(fetch(part, first, width, to, sems.at[2 * n + part]))
    copies.append(fetch(2, 0, FF_LOCAL, wd, sems.at[12]))
    for c in copies:
        c.start()
    res = ffn_rows(x, wg, wd, hidden, copies)
    for i, out in enumerate(outs):
        out[...] = res[64 * i : 64 * i + 64].astype(jnp.bfloat16)


def second_kernel(x, wg, wd, nxt_out, prv_out, own_out, hidden):
    res = ffn_rows(x, wg, wd, hidden)
    nxt_out[...] = res[:64].astype(jnp.bfloat16)
    prv_out[...] = res[64:128].astype(jnp.bfloat16)
    own_out[...] = res[128:]


def bf16(*shape):
    return jax.ShapeDtypeStruct(shape, jnp.bfloat16)


def feed_forward(own, nxt, far_lo, far_hi, prv, weights):
    vmem = pl.BlockSpec(memory_space=pltpu.VMEM)
    hbm = pl.BlockSpec(memory_space=pltpu.HBM)
    half = bf16(64, 2048)
    x1 = jnp.concatenate([far_lo, far_hi, nxt[64:], prv[:64]])
    x2 = jnp.concatenate([nxt[:64], prv[64:], own])
    hidden = pltpu.VMEM((256, FF_LOCAL), jnp.bfloat16)
    limit = pltpu.CompilerParams(vmem_limit_bytes=LIMIT * 1024 * 1024)
    out_lo, out_hi, nxt_hi, prv_lo, wg, wd = pl.pallas_call(
        first_kernel,
        out_shape=(half,) * 4 + (bf16(2048, 2 * FF_LOCAL), bf16(2048, FF_LOCAL)),
        in_specs=[vmem, hbm],
        out_specs=(vmem,) * 6,
        scratch_shapes=[hidden, pltpu.SemaphoreType.DMA((13,))],
        compiler_params=limit,
        name="ffn1",
    )(x1, weights)
    up, down = hop(out_lo, 1), hop(out_hi, -1)
    prev_hi, next_lo = hop(nxt_hi, 1), hop(prv_lo, -1)
    nxt_lo, prv_hi, mine = pl.pallas_call(
        second_kernel,
        out_shape=(half, half, jax.ShapeDtypeStruct((128, 2048), jnp.float32)),
        in_specs=[vmem] * 3,
        out_specs=(vmem,) * 3,
        scratch_shapes=[hidden],
        compiler_params=limit,
        name="ffn2",
    )(x2, wg, wd)
    up_sum = (nxt_lo.astype(jnp.float32) + up.astype(jnp.float32)).astype(jnp.bfloat16)
    down_sum = (prv_hi.astype(jnp.float32) + down.astype(jnp.float32)).astype(jnp.bfloat16)
    prev_lo, next_hi = hop(up_sum, 1), hop(down_sum, -1)
    return mine, prev_lo, prev_hi, next_lo, next_hi


def shards(
    queries,
    key_rows,
    value_rows,
    sink_logits,
    residual,
    norm_gain,
    out_weight,
    gate_weight,
    up_weight,
    down_weight,
):
    tok_local = queries.shape[0]
    block_len = 2 * WIN
    share_rows = tok_local // lax.axis_size("tp")
    seq_len = tok_local * lax.axis_size("sp")
    device_offset = lax.axis_index("sp") * tok_local
    kv_pair = jnp.stack([key_rows, value_rows])
    kv_ext = with_halo(kv_pair, (("sp", 1),), WIN)

    def one_block(block_index):
        block_first = block_index * block_len
        query_blk = lax.dynamic_slice_in_dim(queries, block_first, block_len, 0)
        key_blk = lax.dynamic_slice_in_dim(kv_ext[0], block_first, block_len + 2 * WIN, 0)
        value_blk = lax.dynamic_slice_in_dim(kv_ext[1], block_first, block_len + 2 * WIN, 0)
        query_pos = device_offset + block_first + jnp.arange(block_len, dtype=jnp.int32)
        key_pos = (
            device_offset + block_first - WIN + jnp.arange(block_len + 2 * WIN, dtype=jnp.int32)
        )
        return attend_block(query_blk, key_blk, value_blk, sink_logits, query_pos, key_pos, seq_len)

    blocks = lax.map(one_block, jnp.arange(tok_local // block_len, dtype=jnp.int32))
    attended = blocks.reshape(tok_local, queries.shape[1])
    own_first = lax.axis_index("tp") * share_rows
    picked = attended
    attn_share = ring_sum(
        jnp.dot(picked, out_weight, preferred_element_type=jnp.float32)
        .astype(jnp.bfloat16)
        .reshape(4, share_rows, -1)
    )
    middle_own = (
        lax.dynamic_slice_in_dim(residual, own_first, share_rows, 0).astype(jnp.float32)
        + attn_share
    )
    normed = rms_scale(middle_own, norm_gain)
    prv, nxt = hop(normed, 1), hop(normed, -1)
    far_lo, far_hi = hop(prv[:64], 1), hop(nxt[64:], -1)
    weights = lax.all_gather(
        jnp.concatenate([gate_weight, up_weight, down_weight.T], axis=1), "sp", axis=0, tiled=True
    )
    mine, prev_lo, prev_hi, next_lo, next_hi = feed_forward(
        normed, nxt, far_lo, far_hi, prv, weights
    )
    ffn_share = mine + jnp.concatenate(
        [
            prev_lo.astype(jnp.float32) + next_lo.astype(jnp.float32),
            prev_hi.astype(jnp.float32) + next_hi.astype(jnp.float32),
        ]
    )
    return (middle_own + ffn_share).astype(jnp.bfloat16)


def solution(mesh):
    placed = (
        P("sp", "tp"),
        P("sp", "tp"),
        P("sp", "tp"),
        P("tp"),
        P("sp", None),
        P(),
        P("tp", None),
        P("sp", "tp"),
        P("sp", "tp"),
        P("tp", "sp"),
    )
    return jax.shard_map(
        shards, mesh=mesh, in_specs=placed, out_specs=P(("sp", "tp"), None), check_vma=False
    )
```

```python
import jax
import jax.numpy as jnp
from jax import lax
from jax.experimental import pallas as pl
from jax.experimental.pallas import tpu as pltpu
from jax.sharding import PartitionSpec as P


DH = 128
WIN = 128


EPSILON = 1e-06
MASKED = -1e30


def with_halo(cells, sides, width):
    for axis, dim in sides:
        count = lax.axis_size(axis)
        ends = count - 1
        head = lax.slice_in_dim(cells, 0, width, axis=dim)
        tail = lax.slice_in_dim(cells, cells.shape[dim] - width, cells.shape[dim], axis=dim)
        cells = jnp.concatenate(
            [
                lax.ppermute(tail, axis, [(i, (i + 1) % count) for i in range(ends)]),
                cells,
                lax.ppermute(head, axis, [((i + 1) % count, i) for i in range(ends)]),
            ],
            axis=dim,
        )
    return cells


def attend_block(query_blk, key_blk, value_blk, sink_logits, query_pos, key_pos, seq_len):
    kv_heads = key_blk.shape[1] // DH
    group_size = query_blk.shape[1] // key_blk.shape[1]
    query_four = query_blk.reshape(query_blk.shape[0], kv_heads, group_size, DH)
    key_three = key_blk.reshape(key_blk.shape[0], kv_heads, DH)
    value_three = value_blk.reshape(value_blk.shape[0], kv_heads, DH)
    scores = jnp.einsum(
        "qhgd,khd->hgqk", query_four, key_three, preferred_element_type=jnp.float32
    ) * DH ** (-0.5)
    allowed = (
        (jnp.abs(key_pos[None, :] - query_pos[:, None]) <= WIN)
        & (key_pos[None, :] >= 0)
        & (key_pos[None, :] < seq_len)
    )
    scores = jnp.where(allowed[None, None], scores, MASKED)
    sink_col = sink_logits.reshape(kv_heads, group_size)[:, :, None]
    highest = jnp.maximum(jnp.max(scores, axis=-1), sink_col)
    weights_exp = jnp.exp(scores - highest[..., None])
    denominator = jnp.sum(weights_exp, axis=-1) + jnp.exp(sink_col - highest)
    probabilities = (weights_exp / denominator[..., None]).astype(jnp.bfloat16)
    heads_out = jnp.einsum(
        "hgqk,khd->qhgd", probabilities, value_three, preferred_element_type=jnp.float32
    )
    return heads_out.astype(jnp.bfloat16).reshape(query_blk.shape[0], kv_heads * group_size * DH)


def rms_scale(rows_wide, norm_gain):
    mean_square = jnp.mean(rows_wide * rows_wide, axis=-1, keepdims=True)
    return (rows_wide * lax.rsqrt(mean_square + EPSILON) * norm_gain).astype(jnp.bfloat16)


def hop(value, step):
    size = lax.axis_size("tp")
    return lax.ppermute(value, "tp", [(i, (i + step) % size) for i in range(size)])


def ring_sum(parts):
    half = parts.shape[1] // 2
    me = lax.axis_index("tp")
    own = lax.dynamic_index_in_dim(parts, me, 0, keepdims=False)
    nxt = lax.dynamic_index_in_dim(parts, (me + 1) % 4, 0, keepdims=False)
    prv = lax.dynamic_index_in_dim(parts, (me + 3) % 4, 0, keepdims=False)
    far = lax.dynamic_index_in_dim(parts, (me + 2) % 4, 0, keepdims=False)
    up = hop(far[:half], 1)
    down = hop(far[half:], -1)
    up_sum = (nxt[:half].astype(jnp.float32) + up.astype(jnp.float32)).astype(jnp.bfloat16)
    down_sum = (prv[half:].astype(jnp.float32) + down.astype(jnp.float32)).astype(jnp.bfloat16)
    from_prev = hop(jnp.concatenate([up_sum, nxt[half:]]), 1)
    from_next = hop(jnp.concatenate([prv[:half], down_sum]), -1)
    return (
        own.astype(jnp.float32) + from_prev.astype(jnp.float32) + from_next.astype(jnp.float32)
    )


FF_LOCAL = 1408
LIMIT = 30
STEPS = ((0, 256), (256, 256), (512, 256), (768, 256), (1024, 256), (1280, 128))


def ffn_rows(x, wg, wd, hidden, ready=None):
    x = x[...]
    for n, (first, width) in enumerate(STEPS):
        if ready is not None:
            ready[2 * n].wait()
            ready[2 * n + 1].wait()
        acc = jnp.dot(
            x, wg[:, 2 * first : 2 * (first + width)], preferred_element_type=jnp.float32
        )
        gate = acc[:, :width]
        hid = gate / (1.0 + jnp.exp(-gate)) * acc[:, width:]
        hidden[:, first : first + width] = hid.astype(jnp.bfloat16)
    if ready is not None:
        ready[12].wait()
    return lax.dot_general(
        hidden[...], wd[...], (((1,), (1,)), ((), ())), preferred_element_type=jnp.float32
    )


def first_kernel(x, w, *refs):
    outs, (wg, wd, hidden, sems) = refs[:4], refs[4:]

    def fetch(part, first, width, to, sem):
        src = w.at[:, pl.ds(part * FF_LOCAL + first, width)]
        return pltpu.make_async_copy(src, to, sem)

    copies = []
    for n, (first, width) in enumerate(STEPS):
        for part in range(2):
            to = wg.at[:, pl.ds(2 * first + part * width, width)]
            copies.append(fetch(part, first, width, to, sems.at[2 * n + part]))
    copies.append(fetch(2, 0, FF_LOCAL, wd, sems.at[12]))
    for c in copies:
        c.start()
    res = ffn_rows(x, wg, wd, hidden, copies)
    for i, out in enumerate(outs):
        out[...] = res[64 * i : 64 * i + 64].astype(jnp.bfloat16)


def second_kernel(x, wg, wd, nxt_out, prv_out, own_out, hidden):
    res = ffn_rows(x, wg, wd, hidden)
    nxt_out[...] = res[:64].astype(jnp.bfloat16)
    prv_out[...] = res[64:128].astype(jnp.bfloat16)
    own_out[...] = res[128:]


def bf16(*shape):
    return jax.ShapeDtypeStruct(shape, jnp.bfloat16)


def feed_forward(own, nxt, far_lo, far_hi, prv, weights):
    vmem = pl.BlockSpec(memory_space=pltpu.VMEM)
    hbm = pl.BlockSpec(memory_space=pltpu.HBM)
    half = bf16(64, 2048)
    x1 = jnp.concatenate([far_lo, far_hi, nxt[64:], prv[:64]])
    x2 = jnp.concatenate([nxt[:64], prv[64:], own])
    hidden = pltpu.VMEM((256, FF_LOCAL), jnp.bfloat16)
    limit = pltpu.CompilerParams(vmem_limit_bytes=LIMIT * 1024 * 1024)
    out_lo, out_hi, nxt_hi, prv_lo, wg, wd = pl.pallas_call(
        first_kernel,
        out_shape=(half,) * 4 + (bf16(2048, 2 * FF_LOCAL), bf16(2048, FF_LOCAL)),
        in_specs=[vmem, hbm],
        out_specs=(vmem,) * 6,
        scratch_shapes=[hidden, pltpu.SemaphoreType.DMA((13,))],
        compiler_params=limit,
        name="ffn1",
    )(x1, weights)
    up = hop(out_lo, 1)
    down = hop(out_hi, -1)
    prev_hi = hop(nxt_hi, 1)
    next_lo = hop(prv_lo, -1)
    nxt_lo, prv_hi, mine = pl.pallas_call(
        second_kernel,
        out_shape=(half, half, jax.ShapeDtypeStruct((128, 2048), jnp.float32)),
        in_specs=[vmem] * 3,
        out_specs=(vmem,) * 3,
        scratch_shapes=[hidden],
        compiler_params=limit,
        name="ffn2",
    )(x2, wg, wd)
    up_sum = (nxt_lo.astype(jnp.float32) + up.astype(jnp.float32)).astype(jnp.bfloat16)
    down_sum = (prv_hi.astype(jnp.float32) + down.astype(jnp.float32)).astype(jnp.bfloat16)
    prev_lo, next_hi = hop(up_sum, 1), hop(down_sum, -1)
    return mine, prev_lo, prev_hi, next_lo, next_hi


def shards(
    queries,
    key_rows,
    value_rows,
    sink_logits,
    residual,
    norm_gain,
    out_weight,
    gate_weight,
    up_weight,
    down_weight,
):
    tok_local = queries.shape[0]
    block_len = 2 * WIN
    share_rows = tok_local // lax.axis_size("tp")
    seq_len = tok_local * lax.axis_size("sp")
    device_offset = lax.axis_index("sp") * tok_local
    kv_pair = jnp.stack([key_rows, value_rows])
    kv_ext = with_halo(kv_pair, (("sp", 1),), WIN)

    def one_block(block_index):
        block_first = block_index * block_len
        query_blk = lax.dynamic_slice_in_dim(queries, block_first, block_len, 0)
        key_blk = lax.dynamic_slice_in_dim(kv_ext[0], block_first, block_len + 2 * WIN, 0)
        value_blk = lax.dynamic_slice_in_dim(kv_ext[1], block_first, block_len + 2 * WIN, 0)
        query_pos = device_offset + block_first + jnp.arange(block_len, dtype=jnp.int32)
        key_pos = (
            device_offset + block_first - WIN + jnp.arange(block_len + 2 * WIN, dtype=jnp.int32)
        )
        return attend_block(query_blk, key_blk, value_blk, sink_logits, query_pos, key_pos, seq_len)

    blocks = lax.map(one_block, jnp.arange(tok_local // block_len, dtype=jnp.int32))
    attended = blocks.reshape(tok_local, queries.shape[1])
    own_first = lax.axis_index("tp") * share_rows
    picked = attended
    attn_share = ring_sum(
        jnp.dot(picked, out_weight, preferred_element_type=jnp.float32)
        .astype(jnp.bfloat16)
        .reshape(4, share_rows, -1)
    )
    middle_own = (
        lax.dynamic_slice_in_dim(residual, own_first, share_rows, 0).astype(jnp.float32)
        + attn_share
    )
    normed = rms_scale(middle_own, norm_gain)
    prv, nxt = hop(normed, 1), hop(normed, -1)
    far_lo, far_hi = hop(prv[:64], 1), hop(nxt[64:], -1)
    weights = lax.all_gather(
        jnp.concatenate([gate_weight, up_weight, down_weight.T], axis=1), "sp", axis=0, tiled=True
    )
    mine, prev_lo, prev_hi, next_lo, next_hi = feed_forward(
        normed, nxt, far_lo, far_hi, prv, weights
    )
    ffn_share = mine + jnp.concatenate(
        [
            prev_lo.astype(jnp.float32) + next_lo.astype(jnp.float32),
            prev_hi.astype(jnp.float32) + next_hi.astype(jnp.float32),
        ]
    )
    return (middle_own + ffn_share).astype(jnp.bfloat16)


def solution(mesh):
    placed = (
        P("sp", "tp"),
        P("sp", "tp"),
        P("sp", "tp"),
        P("tp"),
        P("sp", None),
        P(),
        P("tp", None),
        P("sp", "tp"),
        P("sp", "tp"),
        P("tp", "sp"),
    )
    return jax.shard_map(
        shards, mesh=mesh, in_specs=placed, out_specs=P(("sp", "tp"), None), check_vma=False
    )
```

```python
import jax
import jax.numpy as jnp
from jax import lax
from jax.experimental import pallas as pl
from jax.experimental.pallas import tpu as pltpu
from jax.sharding import PartitionSpec as P


DH = 128
WIN = 128


EPSILON = 1e-06
MASKED = -1e30


def with_halo(cells, sides, width):
    for axis, dim in sides:
        count = lax.axis_size(axis)
        ends = count - 1
        head = lax.slice_in_dim(cells, 0, width, axis=dim)
        tail = lax.slice_in_dim(cells, cells.shape[dim] - width, cells.shape[dim], axis=dim)
        cells = jnp.concatenate(
            [
                lax.ppermute(tail, axis, [(i, (i + 1) % count) for i in range(ends)]),
                cells,
                lax.ppermute(head, axis, [((i + 1) % count, i) for i in range(ends)]),
            ],
            axis=dim,
        )
    return cells


def attend_block(query_blk, key_blk, value_blk, sink_logits, query_pos, key_pos, seq_len):
    kv_heads = key_blk.shape[1] // DH
    group_size = query_blk.shape[1] // key_blk.shape[1]
    query_four = query_blk.reshape(query_blk.shape[0], kv_heads, group_size, DH)
    key_three = key_blk.reshape(key_blk.shape[0], kv_heads, DH)
    value_three = value_blk.reshape(value_blk.shape[0], kv_heads, DH)
    scores = jnp.einsum(
        "qhgd,khd->hgqk", query_four, key_three, preferred_element_type=jnp.float32
    ) * DH ** (-0.5)
    allowed = (
        (jnp.abs(key_pos[None, :] - query_pos[:, None]) <= WIN)
        & (key_pos[None, :] >= 0)
        & (key_pos[None, :] < seq_len)
    )
    scores = jnp.where(allowed[None, None], scores, MASKED)
    sink_col = sink_logits.reshape(kv_heads, group_size)[:, :, None]
    highest = jnp.maximum(jnp.max(scores, axis=-1), sink_col)
    weights_exp = jnp.exp(scores - highest[..., None])
    denominator = jnp.sum(weights_exp, axis=-1) + jnp.exp(sink_col - highest)
    probabilities = (weights_exp / denominator[..., None]).astype(jnp.bfloat16)
    heads_out = jnp.einsum(
        "hgqk,khd->qhgd", probabilities, value_three, preferred_element_type=jnp.float32
    )
    return heads_out.astype(jnp.bfloat16).reshape(query_blk.shape[0], kv_heads * group_size * DH)


def rms_scale(rows_wide, norm_gain):
    mean_square = jnp.mean(rows_wide * rows_wide, axis=-1, keepdims=True)
    return (rows_wide * lax.rsqrt(mean_square + EPSILON) * norm_gain).astype(jnp.bfloat16)


def hop(value, step):
    size = lax.axis_size("tp")
    return lax.ppermute(value, "tp", [(i, (i + step) % size) for i in range(size)])


def ring_sum(parts):
    half = parts.shape[1] // 2
    me = lax.axis_index("tp")
    own = lax.dynamic_index_in_dim(parts, me, 0, keepdims=False)
    nxt = lax.dynamic_index_in_dim(parts, (me + 1) % 4, 0, keepdims=False)
    prv = lax.dynamic_index_in_dim(parts, (me + 3) % 4, 0, keepdims=False)
    far = lax.dynamic_index_in_dim(parts, (me + 2) % 4, 0, keepdims=False)
    up = hop(far[:half], 1)
    down = hop(far[half:], -1)
    up_sum = (nxt[:half].astype(jnp.float32) + up.astype(jnp.float32)).astype(jnp.bfloat16)
    down_sum = (prv[half:].astype(jnp.float32) + down.astype(jnp.float32)).astype(jnp.bfloat16)
    from_prev = hop(jnp.concatenate([up_sum, nxt[half:]]), 1)
    from_next = hop(jnp.concatenate([prv[:half], down_sum]), -1)
    return (
        own.astype(jnp.float32) + from_prev.astype(jnp.float32) + from_next.astype(jnp.float32)
    )


FF_LOCAL = 1408
LIMIT = 30
STEPS = ((0, 256), (256, 256), (512, 256), (768, 256), (1024, 256), (1280, 128))


def ffn_rows(x, wg, wd, hidden, ready=None):
    x = x[...]
    for n, (first, width) in enumerate(STEPS):
        if ready is not None:
            ready[2 * n].wait()
            ready[2 * n + 1].wait()
        acc = jnp.dot(
            x, wg[:, 2 * first : 2 * (first + width)], preferred_element_type=jnp.float32
        )
        gate = acc[:, :width]
        hid = gate / (1.0 + jnp.exp(-gate)) * acc[:, width:]
        hidden[:, first : first + width] = hid.astype(jnp.bfloat16)
    if ready is not None:
        ready[12].wait()
    return lax.dot_general(
        hidden[...], wd[...], (((1,), (1,)), ((), ())), preferred_element_type=jnp.float32
    )


def first_kernel(x, w, *refs):
    outs, (wg, wd, hidden, sems) = refs[:4], refs[4:]

    def fetch(part, first, width, to, sem):
        src = w.at[:, pl.ds(part * FF_LOCAL + first, width)]
        return pltpu.make_async_copy(src, to, sem)

    copies = []
    for n, (first, width) in enumerate(STEPS):
        for part in range(2):
            to = wg.at[:, pl.ds(2 * first + part * width, width)]
            copies.append(fetch(part, first, width, to, sems.at[2 * n + part]))
    copies.append(fetch(2, 0, FF_LOCAL, wd, sems.at[12]))
    for c in copies:
        c.start()
    res = ffn_rows(x, wg, wd, hidden, copies)
    for i, out in enumerate(outs):
        out[...] = res[64 * i : 64 * i + 64].astype(jnp.bfloat16)


def second_kernel(x, wg, wd, nxt_out, prv_out, own_out, hidden):
    res = ffn_rows(x, wg, wd, hidden)
    nxt_out[...] = res[:64].astype(jnp.bfloat16)
    prv_out[...] = res[64:128].astype(jnp.bfloat16)
    own_out[...] = res[128:]


def bf16(*shape):
    return jax.ShapeDtypeStruct(shape, jnp.bfloat16)


def feed_forward(own, nxt, far_lo, far_hi, prv, weights):
    vmem = pl.BlockSpec(memory_space=pltpu.VMEM)
    hbm = pl.BlockSpec(memory_space=pltpu.HBM)
    half = bf16(64, 2048)
    x1 = jnp.concatenate([far_lo, far_hi, nxt[64:], prv[:64]])
    x2 = jnp.concatenate([nxt[:64], prv[64:], own])
    hidden = pltpu.VMEM((256, FF_LOCAL), jnp.bfloat16)
    limit = pltpu.CompilerParams(vmem_limit_bytes=LIMIT * 1024 * 1024)
    out_lo, out_hi, nxt_hi, prv_lo, wg, wd = pl.pallas_call(
        first_kernel,
        out_shape=(half,) * 4 + (bf16(2048, 2 * FF_LOCAL), bf16(2048, FF_LOCAL)),
        in_specs=[vmem, hbm],
        out_specs=(vmem,) * 6,
        scratch_shapes=[hidden, pltpu.SemaphoreType.DMA((13,))],
        compiler_params=limit,
        name="ffn1",
    )(x1, weights)
    up = hop(out_lo, 1)
    down = hop(out_hi, -1)
    prev_hi = hop(nxt_hi, 1)
    next_lo = hop(prv_lo, -1)
    nxt_lo, prv_hi, mine = pl.pallas_call(
        second_kernel,
        out_shape=(half, half, jax.ShapeDtypeStruct((128, 2048), jnp.float32)),
        in_specs=[vmem] * 3,
        out_specs=(vmem,) * 3,
        scratch_shapes=[hidden],
        compiler_params=limit,
        name="ffn2",
    )(x2, wg, wd)
    up_sum = (nxt_lo.astype(jnp.float32) + up.astype(jnp.float32)).astype(jnp.bfloat16)
    down_sum = (prv_hi.astype(jnp.float32) + down.astype(jnp.float32)).astype(jnp.bfloat16)
    prev_lo, next_hi = hop(up_sum, 1), hop(down_sum, -1)
    return mine, prev_lo, prev_hi, next_lo, next_hi


def shards(
    queries,
    key_rows,
    value_rows,
    sink_logits,
    residual,
    norm_gain,
    out_weight,
    gate_weight,
    up_weight,
    down_weight,
):
    tok_local = queries.shape[0]
    block_len = 2 * WIN
    share_rows = tok_local // lax.axis_size("tp")
    seq_len = tok_local * lax.axis_size("sp")
    device_offset = lax.axis_index("sp") * tok_local
    kv_pair = jnp.stack([key_rows, value_rows])
    kv_ext = with_halo(kv_pair, (("sp", 1),), WIN)

    def one_block(block_index):
        block_first = block_index * block_len
        query_blk = lax.dynamic_slice_in_dim(queries, block_first, block_len, 0)
        key_blk = lax.dynamic_slice_in_dim(kv_ext[0], block_first, block_len + 2 * WIN, 0)
        value_blk = lax.dynamic_slice_in_dim(kv_ext[1], block_first, block_len + 2 * WIN, 0)
        query_pos = device_offset + block_first + jnp.arange(block_len, dtype=jnp.int32)
        key_pos = (
            device_offset + block_first - WIN + jnp.arange(block_len + 2 * WIN, dtype=jnp.int32)
        )
        return attend_block(query_blk, key_blk, value_blk, sink_logits, query_pos, key_pos, seq_len)

    blocks = lax.map(one_block, jnp.arange(tok_local // block_len, dtype=jnp.int32))
    attended = blocks.reshape(tok_local, queries.shape[1])
    own_first = lax.axis_index("tp") * share_rows
    picked = attended
    attn_share = ring_sum(
        jnp.dot(picked, out_weight, preferred_element_type=jnp.float32)
        .astype(jnp.bfloat16)
        .reshape(4, share_rows, -1)
    )
    middle_own = (
        lax.dynamic_slice_in_dim(residual, own_first, share_rows, 0).astype(jnp.float32)
        + attn_share
    )
    normed = rms_scale(middle_own, norm_gain)
    prv, nxt = hop(normed, 1), hop(normed, -1)
    far_lo, far_hi = hop(prv[:64], 1), hop(nxt[64:], -1)
    weights = lax.all_gather(
        jnp.concatenate([gate_weight, up_weight, down_weight.T], axis=1), "sp", axis=0, tiled=True
    )
    mine, prev_lo, prev_hi, next_lo, next_hi = feed_forward(
        normed, nxt, far_lo, far_hi, prv, weights
    )
    ready = (middle_own + mine) + jnp.concatenate([next_lo, prev_hi]).astype(jnp.float32)
    ready, prev_lo, next_hi = lax.optimization_barrier((ready, prev_lo, next_hi))
    return (ready + jnp.concatenate([prev_lo, next_hi]).astype(jnp.float32)).astype(jnp.bfloat16)


def solution(mesh):
    placed = (
        P("sp", "tp"),
        P("sp", "tp"),
        P("sp", "tp"),
        P("tp"),
        P("sp", None),
        P(),
        P("tp", None),
        P("sp", "tp"),
        P("sp", "tp"),
        P("tp", "sp"),
    )
    return jax.shard_map(
        shards, mesh=mesh, in_specs=placed, out_specs=P(("sp", "tp"), None), check_vma=False
    )
```
